32 devices in a mesh: ep: 8 (over z, y), tp: 4 (over x, core).
Axes of the slice: x: 2, y: 2, z: 4, core: 2. Of those that a mesh axis runs over, the one named last changes fastest.
Arguments:
- tokens: bfloat16 [16, 2048], P('ep'), may hold values from -6 to 6
- state_c: float32 [16, 8, 128, 256], P('ep', 'tp'), may hold values from -0.8 to 0.8
- state_n: float32 [16, 8, 128], P('ep', 'tp'), may hold values from -0.8 to 0.8
- state_m: float32 [16, 8], P('ep', 'tp'), may hold values from -2 to 2
- mix_gain: float32 [2048], replicated, may hold values from 0.1 to 1.9
- w_query: bfloat16 [2048, 1024], P('ep', 'tp'), may hold values from -0.125 to 0.125
- w_key: bfloat16 [2048, 1024], P('ep', 'tp'), may hold values from -0.125 to 0.125
- w_value: bfloat16 [2048, 2048], P('ep', 'tp'), may hold values from -0.125 to 0.125
- w_input_gate: bfloat16 [2048, 8], replicated, may hold values from -0.125 to 0.125
- w_forget_gate: bfloat16 [2048, 8], replicated, may hold values from -0.125 to 0.125
- forget_bias: float32 [8], replicated, may hold values from -1 to 4
- w_output: bfloat16 [2048, 2048], P('tp', 'ep'), may hold values from -0.125 to 0.125
- moe_gain: float32 [2048], replicated, may hold values from 0.1 to 1.9
- w_group: bfloat16 [2048, 4], replicated, may hold values from -0.25 to 0.25
- expert_ids: int32 [16, 2], P('ep'), may hold values from 0 to 7, all different within a row; in each aligned block of 2 rows (0 to 1, 2 to 3, ...) at most 1 rows name the same one
- expert_weight: float32 [16, 2], P('ep'), may hold values from 0.1 to 1
- w_exp_gate: bfloat16 [8, 2048, 512], P('ep', None, 'tp'), may hold values from -0.125 to 0.125
- w_exp_up: bfloat16 [8, 2048, 512], P('ep', None, 'tp'), may hold values from -0.25 to 0.25
- w_exp_down: bfloat16 [8, 512, 2048], P('ep', 'tp'), may hold values from -1 to 1
- w_dense: bfloat16 [2048, 2048], P('ep', 'tp'), may hold values from -0.125 to 0.125
- w_dense_gate: bfloat16 [2048], replicated, may hold values from -0.125 to 0.125
Outputs:
- mixed: bfloat16 [16, 2048], P('ep', 'tp')
- new_c: float32 [16, 8, 128, 256], P('ep', 'tp')
- new_n: float32 [16, 8, 128], P('ep', 'tp')
- new_m: float32 [16, 8], P('ep', 'tp')
The draws below stay inside these ranges and needn't reach their ends.
Inputs may be any that keep to these rules, and one draw needn't show every extreme that they name: `expert_ids`: each row names 2 different experts. In each aligned block of 2 rows (the rows of one index of ep) no expert is named by more than 1 row, a bound that some block reaches. Every expert is named by some row.
All inputs are finite; a program needn't handle non-finite values.
Results may differ from the reference program's by a relative error of at most 0.025.
Values may be sent and summed in bfloat16 or wider, within the bound.
A program may use at most 64 MiB of HBM per device.

```python
import math
import jax
import jax.numpy as jnp
import numpy as np
from jax import lax

D = 2048
HEADS = 8
DQK = 128
DV = 256
FF = 512
GROUPS = 4
TOPK = 2
SEQ_DEV = 2
SEQS = 16
EXPERTS = 8
CAP = 1
N_TP = 4


def block_levels(own_key, shape, cuts, least, top_value):
    loudness, own = 1.0, jax.random.fold_in(own_key, 6)
    for dim, blocks in cuts:
        heights = jnp.exp(jax.random.uniform(jax.random.fold_in(own, dim), (blocks,), jnp.float32, least / len(cuts), top_value / len(cuts)))
        loudness = loudness * jnp.repeat(heights, shape[dim] // blocks).reshape([-1 if axis == dim else 1 for axis in range(len(shape))])
    return loudness


def assign_block(own_key, own, number, rows, count, top, reach, slope):
    order = jax.random.permutation(own_key, count)
    heavy_load, common = load_shares(count, rows * top, reach, slope, True), load_shares(count, rows * top, reach, slope, False)
    places = jnp.arange(count)

    def named(tallies, offset_by):
        used = int((tallies > 0).sum())
        fixed = max(1, used // 4)
        shifted = fixed + (places - fixed + offset_by * (used - fixed)) % max(1, count - fixed)
        return jnp.zeros((count,), jnp.int32).at[order[jnp.where(places < fixed, places, shifted)]].set(jnp.asarray(tallies, jnp.int32))

    tallies = jnp.where(number % 4 == 0, named(heavy_load, number // 4), named(common, number - number // 4 - 1))
    mixed = jax.random.permutation(jax.random.fold_in(own, 3), count)
    source_of, taker = mixed[0:count // 2 * 2:2], mixed[1:count // 2 * 2:2]
    slack = jnp.minimum(tallies[source_of] - 1, reach - tallies[taker]) // 2
    slack = jnp.where((source_of == order[0]) | (taker == order[0]) | (tallies[taker] == 0), 0, jnp.maximum(slack, 0))
    shifted = jax.random.randint(jax.random.fold_in(own, 4), (count // 2,), 0, 1 << 20) % (slack + 1)
    tallies = tallies.at[source_of].add(-shifted).at[taker].add(shifted)
    members = jnp.searchsorted(jnp.cumsum(tallies), jnp.arange(rows * top), side="right").astype(jnp.int32)
    listing = members.reshape(top, rows).T
    listing = listing[jax.random.permutation(jax.random.fold_in(own, 1), rows)]
    offset_by = jax.random.randint(jax.random.fold_in(own, 2), (rows, 1), 0, top)
    return jnp.take_along_axis(listing, (jnp.arange(top)[None, :] + offset_by) % top, axis=1)


def load_shares(count, total, reach, slope, full):
    portions = [(1 << 20) // math.isqrt(grade ** slope) + 1 for grade in range(1, count + 1)]
    largest = reach if full else min(reach, max(-(-total // count), total * portions[0] // sum(portions)))
    least = 1 if total - largest >= count - 1 else 0
    counts, spare = [largest] + [least] * (count - 1), total - largest - least * (count - 1)
    while spare > 0:
        candidates = [i for i in range(1, count) if counts[i] < largest] or [i for i in range(1, count) if counts[i] < reach]
        whole, left = sum([portions[i] for i in candidates]), spare
        for i in candidates:
            more = min(reach - counts[i], max(1, left * portions[i] // whole), spare)
            counts[i] = counts[i] + more
            spare = spare - more
    return np.array(counts)


def gaussian(own_key, dims, scale, limit, shards=(), kind=jnp.bfloat16):
    result = scale * jax.random.normal(own_key, dims, jnp.float32)
    if shards:
        result = result * block_levels(own_key, dims, shards, -0.22, 0.18)
    return jnp.clip(result, -limit, limit).astype(kind)


def setup_inputs(seed: int = 0) -> dict:
    splits = jax.random.split(jax.random.key(seed), 22)
    tokens = gaussian(splits[0], (SEQS, D), 1.0, 6.0, ((0, 8),))
    state_c = gaussian(splits[1], (SEQS, HEADS, DQK, DV), 0.1, 0.8, ((0, 8), (1, 4)), jnp.float32)
    state_n = gaussian(splits[2], (SEQS, HEADS, DQK), 0.1, 0.8, ((0, 8), (1, 4)), jnp.float32)
    state_m = jnp.clip(jax.random.uniform(splits[3], (SEQS, HEADS), jnp.float32, -2.0, 2.0) * block_levels(splits[3], (SEQS, HEADS), ((0, 8), (1, 4)), -0.4, 0.0), -2.0, 2.0)
    mix_gain = jnp.clip(1.0 + 0.18 * jax.random.normal(splits[4], (D,), jnp.float32), 0.1, 1.9)
    w_query = gaussian(splits[5], (D, HEADS * DQK), D ** -0.5, 0.125, ((0, 8), (1, 4)))
    w_key = gaussian(splits[6], (D, HEADS * DQK), D ** -0.5, 0.125, ((0, 8), (1, 4)))
    w_value = gaussian(splits[7], (D, HEADS * DV), D ** -0.5, 0.125, ((0, 8), (1, 4)))
    w_input_gate = gaussian(splits[8], (D, HEADS), D ** -0.5, 0.125)
    w_forget_gate = gaussian(splits[9], (D, HEADS), D ** -0.5, 0.125)
    forget_bias = jnp.clip(jax.random.uniform(splits[10], (HEADS,), jnp.float32, -1.0, 4.0), -1.0, 4.0)
    w_output = gaussian(splits[11], (HEADS * DV, D), (HEADS * DV) ** -0.5, 0.125, ((0, 4), (1, 8)))
    moe_gain = jnp.clip(1.0 + 0.18 * jax.random.normal(splits[12], (D,), jnp.float32), 0.1, 1.9)
    w_group = gaussian(splits[13], (D, GROUPS), (D // 4) ** -0.5, 0.25)
    expert_ids_keys = jax.random.split(jax.random.fold_in(splits[14], 1), SEQS // SEQ_DEV)
    expert_ids_turns = jax.random.permutation(jax.random.fold_in(splits[14], 3), SEQS // SEQ_DEV)
    expert_ids = jax.vmap(lambda own, number: assign_block(jax.random.fold_in(splits[14], 2), own, number, SEQ_DEV, EXPERTS, TOPK, CAP, 2))(expert_ids_keys, expert_ids_turns).reshape((SEQS, TOPK))
    expert_weight = jnp.clip(jnp.exp(math.log(1.0) - 2.3025851 * jax.random.uniform(splits[15], (SEQS, TOPK), jnp.float32) ** block_levels(splits[15], (SEQS, TOPK), ((0, 8),), -0.2, 0.2)), 0.1, 1.0)
    w_exp_gate = gaussian(splits[16], (EXPERTS, D, FF), D ** -0.5, 0.125, ((0, 8), (2, 4)))
    w_exp_up = gaussian(splits[17], (EXPERTS, D, FF), (D // 4) ** -0.5, 0.25, ((0, 8), (2, 4)))
    w_exp_down = gaussian(splits[18], (EXPERTS, FF, D), (FF // 16) ** -0.5, 1.0, ((0, 8), (1, 4)))
    w_dense = gaussian(splits[19], (D, D), D ** -0.5, 0.125, ((0, 8), (1, 4)))
    w_dense_gate = gaussian(splits[20], (D,), D ** -0.5, 0.125)
    return dict(tokens=tokens, state_c=state_c, state_n=state_n, state_m=state_m, mix_gain=mix_gain, w_query=w_query, w_key=w_key, w_value=w_value, w_input_gate=w_input_gate, w_forget_gate=w_forget_gate, forget_bias=forget_bias, w_output=w_output, moe_gain=moe_gain, w_group=w_group, expert_ids=expert_ids, expert_weight=expert_weight, w_exp_gate=w_exp_gate, w_exp_up=w_exp_up, w_exp_down=w_exp_down, w_dense=w_dense, w_dense_gate=w_dense_gate)


eps = 1e-06

def rms_norm(values, gain):
    widened = values.astype(jnp.float32)
    inverse = lax.rsqrt(lax.optimization_barrier(jnp.mean(widened * widened, axis=-1, keepdims=True)) + eps)
    return (widened * inverse * gain).astype(jnp.bfloat16)

def rounded(values):
    return lax.optimization_barrier(values.astype(jnp.bfloat16)).astype(jnp.float32)

def memory_step(query_rows, key_rows, value_rows, in_gate, forget, state_c, state_n, state_m):
    seq_count, head_count = state_m.shape
    q_heads = query_rows.reshape(seq_count, head_count, -1)
    k_heads = key_rows.reshape(seq_count, head_count, -1) * q_heads.shape[-1] ** (-0.5)
    v_heads = value_rows.reshape(seq_count, head_count, -1)
    new_m = jnp.maximum(forget + state_m, in_gate)
    decay = jnp.exp(forget + state_m - new_m)
    inflow = jnp.exp(in_gate - new_m)
    new_c = decay[..., None, None] * state_c + (inflow[..., None] * k_heads)[..., :, None] * v_heads[..., None, :]
    new_n = decay[..., None] * state_n + inflow[..., None] * k_heads
    numer = jnp.einsum('shd,shde->she', q_heads, new_c, precision=lax.Precision.HIGHEST)
    denom = jnp.maximum(jnp.abs(lax.optimization_barrier(jnp.sum(q_heads * new_n, axis=-1))), 1.0)
    heads = (numer / denom[..., None]).astype(jnp.bfloat16).reshape(seq_count, -1)
    return (heads, new_c, new_n, new_m)

def reference(tokens, state_c, state_n, state_m, mix_gain, w_query, w_key, w_value, w_input_gate, w_forget_gate, forget_bias, w_output, moe_gain, w_group, expert_ids, expert_weight, w_exp_gate, w_exp_up, w_exp_down, w_dense, w_dense_gate):
    seq_count = tokens.shape[0]
    normed = rms_norm(tokens, mix_gain)
    query_rows = rounded(jnp.dot(normed, w_query, preferred_element_type=jnp.float32))
    key_rows = rounded(jnp.dot(normed, w_key, preferred_element_type=jnp.float32))
    value_rows = rounded(jnp.dot(normed, w_value, preferred_element_type=jnp.float32))
    in_gate = jnp.dot(normed, w_input_gate, preferred_element_type=jnp.float32)
    forget = jax.nn.log_sigmoid(jnp.dot(normed, w_forget_gate, preferred_element_type=jnp.float32) + forget_bias)
    heads, new_c, new_n, new_m = memory_step(query_rows, key_rows, value_rows, in_gate, forget, state_c, state_n, state_m)
    head_blocks = heads.reshape(seq_count, N_TP, -1).astype(jnp.float32)
    out_blocks = w_output.reshape(N_TP, -1, D).astype(jnp.float32)
    partials = rounded(jnp.einsum('stf,tfd->tsd', head_blocks, out_blocks))
    residual = (tokens.astype(jnp.float32) + lax.optimization_barrier(jnp.sum(partials, axis=0))).astype(jnp.bfloat16)
    normed2 = rms_norm(residual, moe_gain)
    group_prob = jax.nn.softmax(jnp.dot(normed2, w_group, preferred_element_type=jnp.float32), axis=-1)
    per_group = EXPERTS // GROUPS
    member = (expert_ids // per_group)[..., None] == jnp.arange(GROUPS, dtype=jnp.int32)[None, None, :]
    picked = lax.optimization_barrier(jnp.sum(jnp.where(member, group_prob[:, None, :], 0.0), axis=-1))
    route = picked * expert_weight / lax.optimization_barrier(jnp.sum(expert_weight, axis=1, keepdims=True))
    flat_ids = expert_ids.reshape(-1).astype(jnp.int32)
    repeated = jnp.repeat(normed2, TOPK, axis=0)

    def run_one(item):
        ident, token_row = item
        gate_matrix = lax.dynamic_index_in_dim(w_exp_gate, ident, 0, keepdims=False)
        up_matrix = lax.dynamic_index_in_dim(w_exp_up, ident, 0, keepdims=False)
        down_matrix = lax.dynamic_index_in_dim(w_exp_down, ident, 0, keepdims=False)
        gate_act = jnp.dot(token_row[None, :], gate_matrix, preferred_element_type=jnp.float32)
        up_act = jnp.dot(token_row[None, :], up_matrix, preferred_element_type=jnp.float32)
        hidden = (jax.nn.silu(gate_act) * up_act).astype(jnp.bfloat16)
        hidden_blocks = hidden.reshape(N_TP, -1).astype(jnp.float32)
        down_blocks = down_matrix.reshape(N_TP, -1, D).astype(jnp.float32)
        parts = rounded(jnp.einsum('tf,tfd->td', hidden_blocks, down_blocks))
        return lax.optimization_barrier(jnp.sum(parts, axis=0)).astype(jnp.bfloat16)
    expert_out = lax.map(run_one, (flat_ids, repeated))
    moe = lax.optimization_barrier(jnp.sum(route[..., None] * expert_out.astype(jnp.float32).reshape(seq_count, TOPK, D), axis=1))
    dense_gate = jax.nn.sigmoid(jnp.dot(normed2, w_dense_gate, preferred_element_type=jnp.float32))
    dense = dense_gate[:, None] * jnp.dot(normed2, w_dense, preferred_element_type=jnp.float32)
    mixed = (residual.astype(jnp.float32) + moe + dense).astype(jnp.bfloat16)
    return (mixed, new_c, new_n, new_m)
```

```python
import functools

import jax
import jax.numpy as jnp
from jax import lax
from jax.experimental import pallas as pl
from jax.experimental.pallas import tpu as pltpu
from jax.sharding import PartitionSpec as P

CAP = 1


eps = 1e-06


def rms_norm(values, gain):
    widened = values.astype(jnp.float32)
    inverse = lax.rsqrt(jnp.mean(widened * widened, axis=-1, keepdims=True) + eps)
    return (widened * inverse * gain).astype(jnp.bfloat16)


def rounded(values):
    return lax.optimization_barrier(values.astype(jnp.bfloat16)).astype(jnp.float32)


def memory_step(query_rows, key_rows, value_rows, in_gate, forget, state_c, state_n, state_m):
    seq_count, head_count = state_m.shape
    q_heads = query_rows.reshape(seq_count, head_count, -1)
    k_heads = key_rows.reshape(seq_count, head_count, -1) * q_heads.shape[-1] ** (-0.5)
    v_heads = value_rows.reshape(seq_count, head_count, -1)
    new_m = jnp.maximum(forget + state_m, in_gate)
    decay = jnp.exp(forget + state_m - new_m)
    inflow = jnp.exp(in_gate - new_m)
    new_c = (
        decay[..., None, None] * state_c
        + (inflow[..., None] * k_heads)[..., :, None] * v_heads[..., None, :]
    )
    new_n = decay[..., None] * state_n + inflow[..., None] * k_heads
    numer = jnp.einsum("shd,shde->she", q_heads, new_c, precision=lax.Precision.HIGHEST)
    denom = jnp.maximum(jnp.abs(jnp.sum(q_heads * new_n, axis=-1)), 1.0)
    heads = (numer / denom[..., None]).astype(jnp.bfloat16).reshape(seq_count, -1)
    return (heads, new_c, new_n, new_m)


def per_device(
    tokens,
    state_c,
    state_n,
    state_m,
    mix_gain,
    w_query,
    w_key,
    w_value,
    w_input_gate,
    w_forget_gate,
    forget_bias,
    w_output,
    moe_gain,
    w_group,
    expert_ids,
    expert_weight,
    w_exp_gate,
    w_exp_up,
    w_exp_down,
    w_dense,
    w_dense_gate,
):
    seq_count = tokens.shape[0]
    width = tokens.shape[1]
    tp_count = lax.axis_size("tp")
    ep_count = lax.axis_size("ep")
    tp_rank = lax.axis_index("tp")
    head_count = state_m.shape[1]
    qk_cols = w_query.shape[1]
    share = width // tp_count
    normed = rms_norm(tokens, mix_gain)
    spread_cols = lax.all_to_all(normed, "ep", split_axis=1, concat_axis=0, tiled=True)
    joined = jnp.concatenate([w_query, w_key, w_value], axis=1)
    token_rows = spread_cols
    summed = lax.psum_scatter(
        jnp.dot(token_rows, joined, preferred_element_type=jnp.float32),
        "ep",
        scatter_dimension=0,
        tiled=True,
    )
    query_sum = summed[:, :qk_cols]
    key_sum = summed[:, qk_cols : 2 * qk_cols]
    value_sum = summed[:, 2 * qk_cols :]
    query_rows = rounded(query_sum)
    key_rows = rounded(key_sum)
    value_rows = rounded(value_sum)
    gate_all = jnp.dot(normed, w_input_gate, preferred_element_type=jnp.float32)
    forget_all = jax.nn.log_sigmoid(
        jnp.dot(normed, w_forget_gate, preferred_element_type=jnp.float32) + forget_bias
    )
    in_gate = lax.dynamic_slice_in_dim(gate_all, tp_rank * head_count, head_count, 1)
    forget = lax.dynamic_slice_in_dim(forget_all, tp_rank * head_count, head_count, 1)
    heads, new_c, new_n, new_m = memory_step(
        query_rows, key_rows, value_rows, in_gate, forget, state_c, state_n, state_m
    )
    row_parts = jnp.dot(
        lax.all_gather(heads, "ep", axis=0, tiled=True),
        w_output,
        preferred_element_type=jnp.float32,
    ).astype(jnp.bfloat16)
    partial_value = lax.all_to_all(row_parts, "ep", split_axis=0, concat_axis=1, tiled=True).astype(
        jnp.float32
    )
    mixer_sum = lax.psum(partial_value.astype(jnp.bfloat16), "tp").astype(jnp.float32)
    residual = (tokens.astype(jnp.float32) + mixer_sum).astype(jnp.bfloat16)
    normed2 = rms_norm(residual, moe_gain)
    group_count = w_group.shape[1]
    group_prob = jax.nn.softmax(
        jnp.dot(normed2, w_group, preferred_element_type=jnp.float32), axis=-1
    )
    experts_here = w_exp_gate.shape[0]
    expert_count = experts_here * ep_count
    per_group = expert_count // group_count
    top_count = expert_ids.shape[1]
    member = (expert_ids // per_group)[..., None] == jnp.arange(group_count, dtype=jnp.int32)[
        None, None, :
    ]
    picked = jnp.sum(jnp.where(member, group_prob[:, None, :], 0.0), axis=-1)
    route = picked * expert_weight / jnp.sum(expert_weight, axis=1, keepdims=True)
    flat_ids = expert_ids.reshape(-1)
    assigned = flat_ids[:, None] == jnp.arange(expert_count, dtype=jnp.int32)[None, :]
    ranks = jnp.cumsum(assigned.astype(jnp.int32), axis=0) - 1
    own_rank = jnp.sum(jnp.where(assigned, ranks, 0), axis=1)
    slot_index = flat_ids * CAP + own_rank
    placing = (
        jnp.arange(expert_count * CAP, dtype=jnp.int32)[:, None] == slot_index[None, :]
    ).astype(jnp.bfloat16)
    repeated = jnp.repeat(normed2, top_count, axis=0)
    outgoing = jnp.dot(placing, repeated, preferred_element_type=jnp.float32).astype(jnp.bfloat16)
    outgoing = outgoing.reshape(expert_count, CAP, width)
    arrived = lax.all_to_all(outgoing, "ep", split_axis=0, concat_axis=0, tiled=True)
    slots = arrived.shape[1]
    grid_rows = arrived.reshape(ep_count, experts_here, slots, width)
    gate_act = jnp.einsum(
        "sxnd,xdf->sxnf", grid_rows, w_exp_gate, preferred_element_type=jnp.float32
    )
    up_act = jnp.einsum("sxnd,xdf->sxnf", grid_rows, w_exp_up, preferred_element_type=jnp.float32)
    hidden = (jax.nn.silu(gate_act) * up_act).astype(jnp.bfloat16)
    down_part = jnp.einsum("sxnf,xfd->sxnd", hidden, w_exp_down, preferred_element_type=jnp.float32)
    reduced = lax.psum_scatter(
        down_part.astype(jnp.bfloat16), "tp", scatter_dimension=3, tiled=True
    )
    returned = lax.all_to_all(
        reduced.reshape(expert_count, slots, share), "ep", split_axis=0, concat_axis=0, tiled=True
    )
    picked_rows = jnp.einsum(
        "ca,cd->ad",
        placing,
        returned.reshape(expert_count * CAP, share),
        preferred_element_type=jnp.float32,
    )
    moe = jnp.sum(route[..., None] * picked_rows.reshape(seq_count, top_count, share), axis=1)
    dense_cols = lax.all_to_all(normed2, "ep", split_axis=1, concat_axis=0, tiled=True)
    token_rows = dense_cols
    dense_raw = lax.psum_scatter(
        jnp.dot(token_rows, w_dense, preferred_element_type=jnp.float32),
        "ep",
        scatter_dimension=0,
        tiled=True,
    )
    dense_gate = jax.nn.sigmoid(jnp.dot(normed2, w_dense_gate, preferred_element_type=jnp.float32))
    own_cols = lax.dynamic_slice_in_dim(residual, tp_rank * share, share, 1).astype(jnp.float32)
    mixed = (own_cols + moe + dense_gate[:, None] * dense_raw).astype(jnp.bfloat16)
    return (mixed, new_c, new_n, new_m)


F32 = jnp.float32
BF16 = jnp.bfloat16
MESH = pl.DeviceIdType.MESH


def fits(ep, tp, args):
    tokens, state_c, w_query, w_exp_gate = args[0], args[1], args[5], args[16]
    seqs, width = tokens.shape
    dqk, dv = state_c.shape[2:]
    return (
        width % (ep * 128) == 0
        and ep % tp == 0
        and w_query.shape[1] % 128 == 0
        and dqk % 128 == 0
        and dv % 128 == 0
        and (width // tp) % 128 == 0
        and w_exp_gate.shape[0] == 1
        and w_exp_gate.shape[2] % 128 == 0
        and seqs == 2
    )


def step_kernel(
    ep,
    tp,
    tokens,
    state_c,
    state_n,
    state_m,
    mix_gain,
    w_query,
    w_key,
    w_value,
    w_in_t,
    w_forget_t,
    forget_bias,
    w_output,
    moe_gain,
    w_group_t,
    ids,
    weight,
    w_gate,
    w_up,
    w_down,
    w_dense,
    w_dense_gate,
    mixed,
    out_c,
    out_n,
    out_m,
    v_c,
    v_qkv,
    v_out,
    v_gu,
    v_down,
    v_dense,
    new_c,
    send_a,
    recv_a,
    send_b,
    recv_b,
    send_c,
    recv_c,
    send_d,
    recv_d,
    blocks,
    send_g,
    recv_g,
    send_f,
    recv_f,
    rows_scr,
    small_scr,
    local_sem,
    ep_send,
    ep_recv,
    tp_send,
    tp_recv,
    f_send,
    f_recv,
):
    me = lax.axis_index("ep")
    mt = lax.axis_index("tp")
    seqs, width = tokens.shape
    heads = state_c.shape[1]
    dqk, dv = state_c.shape[2:]
    qk = heads * dqk
    col = width // ep
    share = width // tp
    ff = w_gate.shape[2]
    every = ep * seqs

    copies = {}
    plan = [
        ("q", w_query, v_qkv.at[:, 0:qk]),
        ("k", w_key, v_qkv.at[:, qk : 2 * qk]),
        ("v", w_value, v_qkv.at[:, 2 * qk :]),
        ("c", state_c, v_c),
        ("o", w_output, v_out),
        ("d", w_dense, v_dense),
        ("g", w_gate.at[0], v_gu.at[:, 0:ff]),
        ("u", w_up.at[0], v_gu.at[:, ff:]),
        ("w", w_down.at[0], v_down),
    ]
    for number, (name, src, dst) in enumerate(plan):
        copies[name] = pltpu.make_async_copy(src, dst, local_sem.at[number])
        copies[name].start()

    barrier = pltpu.get_barrier_semaphore()
    for k in range(ep):
        for j in range(tp):
            if k or j:
                pl.semaphore_signal(
                    barrier,
                    inc=1,
                    device_id={"ep": lax.rem(me + k, ep), "tp": lax.rem(mt + j, tp)},
                    device_id_type=MESH,
                )

    def to_ep(phase, k, src, dst):
        return pltpu.make_async_remote_copy(
            src_ref=src,
            dst_ref=dst,
            send_sem=ep_send.at[phase, k],
            recv_sem=ep_recv.at[phase, k],
            device_id={"ep": lax.rem(me + k, ep), "tp": mt},
            device_id_type=MESH,
        )

    def source(k):
        return lax.rem(me + (ep - k), ep)

    sends = []
    tok = tokens[...].astype(F32)
    inverse = lax.rsqrt(jnp.mean(tok * tok, axis=-1, keepdims=True) + eps)
    normed_f = tok * inverse * mix_gain[...]
    normed = normed_f.astype(BF16)
    both = jnp.concatenate([normed.astype(F32), tok], axis=0).astype(BF16)
    for e in range(ep):
        send_a[e] = both[:, e * col : (e + 1) * col]
    recv_a[me] = send_a[me]

    pl.semaphore_wait(barrier, ep * tp - 1)

    order = sorted(range(1, ep), key=lambda k: -min(k, ep - k))
    near = order[::-1]
    for k in order:
        copy = to_ep(0, k, send_a.at[lax.rem(me + k, ep)], recv_a.at[me])
        copy.start()
        sends.append(copy)

    last = (((1,), (1,)), ((), ()))
    gate_all = lax.dot_general(normed, w_in_t[...], last, preferred_element_type=F32)
    pre = lax.dot_general(normed, w_forget_t[...], last, preferred_element_type=F32)
    pre = pre + forget_bias[...]
    forget_all = jnp.minimum(pre, 0.0) - jnp.log1p(jnp.exp(-jnp.abs(pre)))
    lane = lax.broadcasted_iota(jnp.int32, gate_all.shape, 1)
    decays, inflows, new_ms = [], [], []
    for h in range(heads):
        here = lane == mt * heads + h
        in_gate = jnp.sum(jnp.where(here, gate_all, 0.0), axis=1, keepdims=True)
        forget = jnp.sum(jnp.where(here, forget_all, 0.0), axis=1, keepdims=True)
        kept = forget + state_m[:, h : h + 1]
        top = jnp.maximum(kept, in_gate)
        new_ms.append(top)
        decays.append(jnp.exp(kept - top))
        inflows.append(jnp.exp(in_gate - top))
    for h in range(heads):
        out_m[:, h : h + 1] = new_ms[h]

    def piece(total, e):
        return total[e * seqs : (e + 1) * seqs]

    for name in ("q", "k", "v"):
        copies[name].wait()
    for k in near:
        to_ep(0, k, send_a.at[0], recv_a.at[source(k)]).wait_recv()
    arrived = [recv_a[e].astype(F32) for e in range(ep)]
    rows = jnp.concatenate([a[:seqs] for a in arrived], axis=0).astype(BF16)
    own_cols = jnp.concatenate([a[seqs:] for a in arrived], axis=0)
    part = jnp.dot(rows, v_qkv[...], preferred_element_type=F32)
    for e in range(ep):
        send_b[e] = piece(part, e).astype(BF16)
    recv_b[me] = send_b[me]
    for k in order:
        copy = to_ep(1, k, send_b.at[lax.rem(me + k, ep)], recv_b.at[me])
        copy.start()
        sends.append(copy)

    copies["c"].wait()
    for k in near:
        to_ep(1, k, send_b.at[0], recv_b.at[source(k)]).wait_recv()
    summed = recv_b[0].astype(F32)
    for e in range(1, ep):
        summed = summed + recv_b[e].astype(F32)
    summed = summed.astype(BF16).astype(F32)
    q_rows, k_rows, v_rows = [], [], []
    for s in range(seqs):
        for h in range(heads):
            row = summed[s : s + 1]
            q_rows.append(row[:, h * dqk : (h + 1) * dqk])
            k_rows.append(
                row[:, qk + h * dqk : qk + (h + 1) * dqk]
                * (dqk ** (-0.5) * inflows[h][s : s + 1])
            )
            v_rows.append(row[:, 2 * qk + h * dv : 2 * qk + (h + 1) * dv])
    upright = jnp.concatenate(q_rows + k_rows, axis=0).T
    count = seqs * heads
    head_rows = []
    for s in range(seqs):
        parts = []
        for h in range(heads):
            at = s * heads + h
            decay = decays[h][s : s + 1]
            q_col = upright[:, at : at + 1]
            k_col = upright[:, count + at : count + at + 1]
            fresh = decay * v_c[s, h] + k_col * v_rows[at]
            new_c[s, h] = fresh
            numer = jnp.sum(q_col * fresh, axis=0, keepdims=True)
            fresh_n = decay * state_n[s, h : h + 1] + k_rows[at]
            out_n[s, h : h + 1] = fresh_n
            denom = jnp.sum(q_rows[at] * fresh_n, axis=1, keepdims=True)
            parts.append(numer / jnp.maximum(jnp.abs(denom), 1.0))
        head_rows.append(jnp.concatenate(parts, axis=1))
    head_out = jnp.concatenate(head_rows, axis=0).astype(BF16)
    send_c[...] = head_out
    recv_c[me] = head_out
    for k in order:
        copy = to_ep(2, k, send_c, recv_c.at[me])
        copy.start()
        sends.append(copy)
    write_c = pltpu.make_async_copy(new_c, out_c, local_sem.at[len(plan)])
    write_c.start()

    small = jnp.concatenate(
        [
            w_group_t[...].astype(F32),
            w_dense_gate[...].astype(F32),
            jnp.zeros((8 - w_group_t.shape[0] - 1, width), F32),
        ],
        axis=0,
    ).astype(BF16)
    small_scr[...] = small

    copies["o"].wait()
    for k in near:
        to_ep(2, k, send_c, recv_c.at[source(k)]).wait_recv()
    all_heads = jnp.concatenate([recv_c[e].astype(F32) for e in range(ep)], axis=0).astype(BF16)
    out_part = jnp.dot(all_heads, v_out[...], preferred_element_type=F32).astype(BF16)
    send_d[...] = out_part
    recv_d[mt] = out_part

    def to_tp(j, dst):
        return pltpu.make_async_remote_copy(
            src_ref=send_d,
            dst_ref=dst,
            send_sem=tp_send.at[j],
            recv_sem=tp_recv.at[j],
            device_id={"ep": me, "tp": lax.rem(mt + j, tp)},
            device_id_type=MESH,
        )

    for j in range(1, tp):
        copy = to_tp(j, recv_d.at[mt])
        copy.start()
        sends.append(copy)
    for j in range(1, tp):
        to_tp(j, recv_d.at[lax.rem(mt + (tp - j), tp)]).wait_recv()
    mixer = recv_d[0].astype(F32)
    for j in range(1, tp):
        mixer = mixer + recv_d[j].astype(F32)
    residual = (own_cols + mixer).astype(BF16)
    blocks[me] = residual
    for k in order:
        copy = to_ep(3, k, blocks.at[me], blocks.at[me])
        copy.start()
        sends.append(copy)

    def gain_of(e):
        return moe_gain[:, pl.ds(pl.multiple_of(e * col, 128), col)]

    copies["d"].wait()
    scaled = (residual.astype(F32) * gain_of(me)).astype(BF16)
    dense_part = jnp.dot(scaled, v_dense[...], preferred_element_type=F32)
    for e in range(ep):
        send_g[e] = piece(dense_part, e).astype(BF16)
    recv_g[me] = send_g[me]
    for k in order:
        copy = to_ep(4, k, send_g.at[lax.rem(me + k, ep)], recv_g.at[me])
        copy.start()
        sends.append(copy)

    for name in ("g", "u", "w"):
        copies[name].wait()

    def block_terms(e, block):
        wide = block.astype(F32)
        squares = jnp.sum(wide * wide, axis=1, keepdims=True)
        scaled = (wide * gain_of(e)).astype(BF16)
        first = pl.multiple_of(e * col, 128)
        act = jnp.dot(scaled, v_gu[pl.ds(first, col), :], preferred_element_type=F32)
        logit = lax.dot_general(
            scaled, small_scr[:, pl.ds(first, col)], last, preferred_element_type=F32
        )
        return squares, act, logit

    squares, act, logit = block_terms(me, residual)
    for k in near:
        e = source(k)
        to_ep(3, k, blocks.at[me], blocks.at[e]).wait_recv()
        more = block_terms(e, blocks[e])
        squares, act, logit = squares + more[0], act + more[1], logit + more[2]
    factor = lax.rsqrt(squares * (1.0 / width) + eps)
    act = act * factor
    gate = act[:, :ff]
    hidden = (gate * jax.nn.sigmoid(gate) * act[:, ff:]).astype(BF16)
    down = jnp.dot(hidden, v_down[...], preferred_element_type=F32)
    for e in range(ep):
        for j in range(tp):
            send_f[e, j] = piece(down, e)[:, j * share : (j + 1) * share].astype(BF16)

    def final(k, j, dst):
        return pltpu.make_async_remote_copy(
            src_ref=send_f.at[lax.rem(me + k, ep), lax.rem(mt + j, tp)],
            dst_ref=dst,
            send_sem=f_send.at[k, j],
            recv_sem=f_recv.at[k, j],
            device_id={"ep": lax.rem(me + k, ep), "tp": lax.rem(mt + j, tp)},
            device_id_type=MESH,
        )

    for k in order + [0]:
        for j in range(tp):
            if k or j:
                copy = final(k, j, recv_f.at[me, mt])
                copy.start()
                sends.append(copy)
    recv_f[me, mt] = send_f[me, mt]

    groups = w_group_t.shape[0]
    spread = jnp.concatenate(
        [logit * factor, factor, jnp.zeros((every, 128 - 9), F32)]
        + [blocks[mt * (share // col) + i].astype(F32) for i in range(share // col)],
        axis=1,
    )
    for e in range(ep):
        rows_scr[e] = piece(spread, e)
    own = rows_scr[me]
    group_logit = own[:, :groups]
    dense_gate = jax.nn.sigmoid(own[:, groups : groups + 1]) * own[:, 8:9]
    shifted = jnp.exp(group_logit - jnp.max(group_logit, axis=1, keepdims=True))
    prob = shifted / jnp.sum(shifted, axis=1, keepdims=True)
    group_lane = lax.broadcasted_iota(jnp.int32, prob.shape, 1)
    per_group = ep // groups
    top_count = ids.shape[1]
    weights = weight[...]
    total_weight = jnp.sum(weights, axis=1, keepdims=True)
    lane_e = lax.broadcasted_iota(jnp.int32, (seqs, ep), 1)
    factor_e = jnp.zeros((seqs, ep), F32)
    for j in range(top_count):
        ident = ids[:, j : j + 1]
        picked = jnp.zeros((seqs, 1), F32)
        for g in range(groups):
            inside = (ident >= g * per_group) & (ident < (g + 1) * per_group)
            picked = picked + jnp.where(inside, prob[:, g : g + 1], 0.0)
        route = picked * weights[:, j : j + 1] / total_weight
        factor_e = factor_e + jnp.where(lane_e == ident, route, 0.0)

    for k in near:
        to_ep(4, k, send_g.at[0], recv_g.at[source(k)]).wait_recv()
    dense = recv_g[0].astype(F32)
    for e in range(1, ep):
        dense = dense + recv_g[e].astype(F32)
    result = own[:, 128:] + dense_gate * dense

    for k in [0] + near:
        for j in range(tp):
            if k or j:
                final(k, j, recv_f.at[source(k), lax.rem(mt + (tp - j), tp)]).wait_recv()
    for e in range(ep):
        expert = recv_f[e, 0].astype(F32)
        for j in range(1, tp):
            expert = expert + recv_f[e, j].astype(F32)
        result = result + factor_e[:, e : e + 1] * expert.astype(BF16).astype(F32)
    mixed[...] = result.astype(BF16)

    write_c.wait()
    for copy in sends:
        copy.wait_send()


def fused(ep, tp, *args):
    (tokens, state_c, state_n, state_m, mix_gain, w_query, w_key, w_value) = args[:8]
    (w_in, w_forget, forget_bias, w_output, moe_gain, w_group, ids, weight) = args[8:16]
    (w_gate, w_up, w_down, w_dense, w_dense_gate) = args[16:]
    seqs, width = tokens.shape
    qk, vals = w_query.shape[1], w_value.shape[1]
    col, share, ff = width // ep, width // tp, w_gate.shape[2]
    every = seqs * ep
    wide = 2 * qk + vals
    vmem = pl.BlockSpec(memory_space=pltpu.VMEM)
    hbm = pl.BlockSpec(memory_space=pl.ANY)
    operands = [
        (tokens, vmem),
        (state_c, hbm),
        (state_n, vmem),
        (state_m, vmem),
        (mix_gain.reshape(1, width), vmem),
        (w_query, hbm),
        (w_key, hbm),
        (w_value, hbm),
        (w_in.T, vmem),
        (w_forget.T, vmem),
        (forget_bias.reshape(1, -1), vmem),
        (w_output, hbm),
        (moe_gain.reshape(1, width), vmem),
        (w_group.T, vmem),
        (ids, vmem),
        (weight, vmem),
        (w_gate, hbm),
        (w_up, hbm),
        (w_down, hbm),
        (w_dense, hbm),
        (w_dense_gate.reshape(1, width), vmem),
    ]
    scratch = [
        pltpu.VMEM(state_c.shape, F32),
        pltpu.VMEM((col, wide), BF16),
        pltpu.VMEM(w_output.shape, BF16),
        pltpu.VMEM((width, 2 * ff), BF16),
        pltpu.VMEM((ff, width), BF16),
        pltpu.VMEM(w_dense.shape, BF16),
        pltpu.VMEM(state_c.shape, F32),
        pltpu.VMEM((ep, 2 * seqs, col), BF16),
        pltpu.VMEM((ep, 2 * seqs, col), BF16),
        pltpu.VMEM((ep, seqs, wide), BF16),
        pltpu.VMEM((ep, seqs, wide), BF16),
        pltpu.VMEM((seqs, vals), BF16),
        pltpu.VMEM((ep, seqs, vals), BF16),
        pltpu.VMEM((every, col), BF16),
        pltpu.VMEM((tp, every, col), BF16),
        pltpu.VMEM((ep, every, col), BF16),
        pltpu.VMEM((ep, seqs, share), BF16),
        pltpu.VMEM((ep, seqs, share), BF16),
        pltpu.VMEM((ep, tp, seqs, share), BF16),
        pltpu.VMEM((ep, tp, seqs, share), BF16),
        pltpu.VMEM((ep, seqs, 128 + share), F32),
        pltpu.VMEM((8, width), BF16),
        pltpu.SemaphoreType.DMA((10,)),
        pltpu.SemaphoreType.DMA((5, ep)),
        pltpu.SemaphoreType.DMA((5, ep)),
        pltpu.SemaphoreType.DMA((tp,)),
        pltpu.SemaphoreType.DMA((tp,)),
        pltpu.SemaphoreType.DMA((ep, tp)),
        pltpu.SemaphoreType.DMA((ep, tp)),
    ]
    return pl.pallas_call(
        functools.partial(step_kernel, ep, tp),
        out_shape=(
            jax.ShapeDtypeStruct((seqs, share), BF16),
            jax.ShapeDtypeStruct(state_c.shape, F32),
            jax.ShapeDtypeStruct(state_n.shape, F32),
            jax.ShapeDtypeStruct(state_m.shape, F32),
        ),
        in_specs=[spec for _, spec in operands],
        out_specs=(vmem, hbm, vmem, vmem),
        scratch_shapes=scratch,
        compiler_params=pltpu.CompilerParams(collective_id=0, has_side_effects=True),
    )(*[value for value, _ in operands])


def solution(mesh):
    ep, tp = mesh.shape["ep"], mesh.shape["tp"]

    def body(*args):
        return fused(ep, tp, *args) if fits(ep, tp, args) else per_device(*args)

    placed = (
        P("ep", None),
        P("ep", "tp", None, None),
        P("ep", "tp", None),
        P("ep", "tp"),
        P(),
        P("ep", "tp"),
        P("ep", "tp"),
        P("ep", "tp"),
        P(),
        P(),
        P(),
        P("tp", "ep"),
        P(),
        P(),
        P("ep", None),
        P("ep", None),
        P("ep", None, "tp"),
        P("ep", None, "tp"),
        P("ep", "tp", None),
        P("ep", "tp"),
        P(),
    )
    return jax.shard_map(
        body,
        mesh=mesh,
        in_specs=placed,
        out_specs=(P("ep", "tp"), P("ep", "tp", None, None), P("ep", "tp", None), P("ep", "tp")),
        check_vma=False,
    )
```

```python
import functools

import jax
import jax.numpy as jnp
from jax import lax
from jax.experimental import pallas as pl
from jax.experimental.pallas import tpu as pltpu
from jax.sharding import PartitionSpec as P

CAP = 1


eps = 1e-06


def rms_norm(values, gain):
    widened = values.astype(jnp.float32)
    inverse = lax.rsqrt(jnp.mean(widened * widened, axis=-1, keepdims=True) + eps)
    return (widened * inverse * gain).astype(jnp.bfloat16)


def rounded(values):
    return lax.optimization_barrier(values.astype(jnp.bfloat16)).astype(jnp.float32)


def memory_step(query_rows, key_rows, value_rows, in_gate, forget, state_c, state_n, state_m):
    seq_count, head_count = state_m.shape
    q_heads = query_rows.reshape(seq_count, head_count, -1)
    k_heads = key_rows.reshape(seq_count, head_count, -1) * q_heads.shape[-1] ** (-0.5)
    v_heads = value_rows.reshape(seq_count, head_count, -1)
    new_m = jnp.maximum(forget + state_m, in_gate)
    decay = jnp.exp(forget + state_m - new_m)
    inflow = jnp.exp(in_gate - new_m)
    new_c = (
        decay[..., None, None] * state_c
        + (inflow[..., None] * k_heads)[..., :, None] * v_heads[..., None, :]
    )
    new_n = decay[..., None] * state_n + inflow[..., None] * k_heads
    numer = jnp.einsum("shd,shde->she", q_heads, new_c, precision=lax.Precision.HIGHEST)
    denom = jnp.maximum(jnp.abs(jnp.sum(q_heads * new_n, axis=-1)), 1.0)
    heads = (numer / denom[..., None]).astype(jnp.bfloat16).reshape(seq_count, -1)
    return (heads, new_c, new_n, new_m)


def per_device(
    tokens,
    state_c,
    state_n,
    state_m,
    mix_gain,
    w_query,
    w_key,
    w_value,
    w_input_gate,
    w_forget_gate,
    forget_bias,
    w_output,
    moe_gain,
    w_group,
    expert_ids,
    expert_weight,
    w_exp_gate,
    w_exp_up,
    w_exp_down,
    w_dense,
    w_dense_gate,
):
    seq_count = tokens.shape[0]
    width = tokens.shape[1]
    tp_count = lax.axis_size("tp")
    ep_count = lax.axis_size("ep")
    tp_rank = lax.axis_index("tp")
    head_count = state_m.shape[1]
    qk_cols = w_query.shape[1]
    share = width // tp_count
    normed = rms_norm(tokens, mix_gain)
    spread_cols = lax.all_to_all(normed, "ep", split_axis=1, concat_axis=0, tiled=True)
    joined = jnp.concatenate([w_query, w_key, w_value], axis=1)
    token_rows = spread_cols
    summed = lax.psum_scatter(
        jnp.dot(token_rows, joined, preferred_element_type=jnp.float32),
        "ep",
        scatter_dimension=0,
        tiled=True,
    )
    query_sum = summed[:, :qk_cols]
    key_sum = summed[:, qk_cols : 2 * qk_cols]
    value_sum = summed[:, 2 * qk_cols :]
    query_rows = rounded(query_sum)
    key_rows = rounded(key_sum)
    value_rows = rounded(value_sum)
    gate_all = jnp.dot(normed, w_input_gate, preferred_element_type=jnp.float32)
    forget_all = jax.nn.log_sigmoid(
        jnp.dot(normed, w_forget_gate, preferred_element_type=jnp.float32) + forget_bias
    )
    in_gate = lax.dynamic_slice_in_dim(gate_all, tp_rank * head_count, head_count, 1)
    forget = lax.dynamic_slice_in_dim(forget_all, tp_rank * head_count, head_count, 1)
    heads, new_c, new_n, new_m = memory_step(
        query_rows, key_rows, value_rows, in_gate, forget, state_c, state_n, state_m
    )
    row_parts = jnp.dot(
        lax.all_gather(heads, "ep", axis=0, tiled=True),
        w_output,
        preferred_element_type=jnp.float32,
    ).astype(jnp.bfloat16)
    partial_value = lax.all_to_all(row_parts, "ep", split_axis=0, concat_axis=1, tiled=True).astype(
        jnp.float32
    )
    mixer_sum = lax.psum(partial_value.astype(jnp.bfloat16), "tp").astype(jnp.float32)
    residual = (tokens.astype(jnp.float32) + mixer_sum).astype(jnp.bfloat16)
    normed2 = rms_norm(residual, moe_gain)
    group_count = w_group.shape[1]
    group_prob = jax.nn.softmax(
        jnp.dot(normed2, w_group, preferred_element_type=jnp.float32), axis=-1
    )
    experts_here = w_exp_gate.shape[0]
    expert_count = experts_here * ep_count
    per_group = expert_count // group_count
    top_count = expert_ids.shape[1]
    member = (expert_ids // per_group)[..., None] == jnp.arange(group_count, dtype=jnp.int32)[
        None, None, :
    ]
    picked = jnp.sum(jnp.where(member, group_prob[:, None, :], 0.0), axis=-1)
    route = picked * expert_weight / jnp.sum(expert_weight, axis=1, keepdims=True)
    flat_ids = expert_ids.reshape(-1)
    assigned = flat_ids[:, None] == jnp.arange(expert_count, dtype=jnp.int32)[None, :]
    ranks = jnp.cumsum(assigned.astype(jnp.int32), axis=0) - 1
    own_rank = jnp.sum(jnp.where(assigned, ranks, 0), axis=1)
    slot_index = flat_ids * CAP + own_rank
    placing = (
        jnp.arange(expert_count * CAP, dtype=jnp.int32)[:, None] == slot_index[None, :]
    ).astype(jnp.bfloat16)
    repeated = jnp.repeat(normed2, top_count, axis=0)
    outgoing = jnp.dot(placing, repeated, preferred_element_type=jnp.float32).astype(jnp.bfloat16)
    outgoing = outgoing.reshape(expert_count, CAP, width)
    arrived = lax.all_to_all(outgoing, "ep", split_axis=0, concat_axis=0, tiled=True)
    slots = arrived.shape[1]
    grid_rows = arrived.reshape(ep_count, experts_here, slots, width)
    gate_act = jnp.einsum(
        "sxnd,xdf->sxnf", grid_rows, w_exp_gate, preferred_element_type=jnp.float32
    )
    up_act = jnp.einsum("sxnd,xdf->sxnf", grid_rows, w_exp_up, preferred_element_type=jnp.float32)
    hidden = (jax.nn.silu(gate_act) * up_act).astype(jnp.bfloat16)
    down_part = jnp.einsum("sxnf,xfd->sxnd", hidden, w_exp_down, preferred_element_type=jnp.float32)
    reduced = lax.psum_scatter(
        down_part.astype(jnp.bfloat16), "tp", scatter_dimension=3, tiled=True
    )
    returned = lax.all_to_all(
        reduced.reshape(expert_count, slots, share), "ep", split_axis=0, concat_axis=0, tiled=True
    )
    picked_rows = jnp.einsum(
        "ca,cd->ad",
        placing,
        returned.reshape(expert_count * CAP, share),
        preferred_element_type=jnp.float32,
    )
    moe = jnp.sum(route[..., None] * picked_rows.reshape(seq_count, top_count, share), axis=1)
    dense_cols = lax.all_to_all(normed2, "ep", split_axis=1, concat_axis=0, tiled=True)
    token_rows = dense_cols
    dense_raw = lax.psum_scatter(
        jnp.dot(token_rows, w_dense, preferred_element_type=jnp.float32),
        "ep",
        scatter_dimension=0,
        tiled=True,
    )
    dense_gate = jax.nn.sigmoid(jnp.dot(normed2, w_dense_gate, preferred_element_type=jnp.float32))
    own_cols = lax.dynamic_slice_in_dim(residual, tp_rank * share, share, 1).astype(jnp.float32)
    mixed = (own_cols + moe + dense_gate[:, None] * dense_raw).astype(jnp.bfloat16)
    return (mixed, new_c, new_n, new_m)


F32 = jnp.float32
BF16 = jnp.bfloat16
MESH = pl.DeviceIdType.MESH


def fits(ep, tp, args):
    tokens, state_c, w_query, w_exp_gate = args[0], args[1], args[5], args[16]
    seqs, width = tokens.shape
    dqk, dv = state_c.shape[2:]
    return (
        width % (ep * 128) == 0
        and ep % tp == 0
        and w_query.shape[1] % 128 == 0
        and dqk % 128 == 0
        and dv % 128 == 0
        and (width // tp) % 128 == 0
        and w_exp_gate.shape[0] == 1
        and w_exp_gate.shape[2] % 128 == 0
        and seqs == 2
    )


def step_kernel(
    ep,
    tp,
    tokens,
    state_c,
    state_n,
    state_m,
    mix_gain,
    w_query,
    w_key,
    w_value,
    w_in_t,
    w_forget_t,
    forget_bias,
    w_output,
    moe_gain,
    w_group_t,
    ids,
    weight,
    w_gate,
    w_up,
    w_down,
    w_dense,
    w_dense_gate,
    mixed,
    out_c,
    out_n,
    out_m,
    v_c,
    v_qkv,
    v_out,
    v_gu,
    v_down,
    v_dense,
    send_a,
    recv_a,
    send_b,
    recv_b,
    send_c,
    recv_c,
    send_d,
    recv_d,
    blocks,
    send_g,
    recv_g,
    send_f,
    recv_f,
    rows_scr,
    small_scr,
    local_sem,
    ep_send,
    ep_recv,
    tp_send,
    tp_recv,
    f_send,
    f_recv,
):
    me = lax.axis_index("ep")
    mt = lax.axis_index("tp")
    seqs, width = tokens.shape
    heads = state_c.shape[1]
    dqk, dv = state_c.shape[2:]
    qk = heads * dqk
    col = width // ep
    share = width // tp
    ff = w_gate.shape[2]
    every = ep * seqs

    copies = {}
    plan = [
        ("q", w_query, v_qkv.at[:, 0:qk]),
        ("k", w_key, v_qkv.at[:, qk : 2 * qk]),
        ("v", w_value, v_qkv.at[:, 2 * qk :]),
        ("c", state_c, v_c),
        ("o", w_output, v_out),
        ("d", w_dense, v_dense),
        ("g", w_gate.at[0], v_gu.at[:, 0:ff]),
        ("u", w_up.at[0], v_gu.at[:, ff:]),
        ("w", w_down.at[0], v_down),
    ]
    for number, (name, src, dst) in enumerate(plan):
        copies[name] = pltpu.make_async_copy(src, dst, local_sem.at[number])
        copies[name].start()

    barrier = pltpu.get_barrier_semaphore()
    for k in range(ep):
        for j in range(tp):
            if k or j:
                pl.semaphore_signal(
                    barrier,
                    inc=1,
                    device_id={"ep": lax.rem(me + k, ep), "tp": lax.rem(mt + j, tp)},
                    device_id_type=MESH,
                )

    def to_ep(phase, k, src, dst):
        return pltpu.make_async_remote_copy(
            src_ref=src,
            dst_ref=dst,
            send_sem=ep_send.at[phase, k],
            recv_sem=ep_recv.at[phase, k],
            device_id={"ep": lax.rem(me + k, ep), "tp": mt},
            device_id_type=MESH,
        )

    def source(k):
        return lax.rem(me + (ep - k), ep)

    sends = []
    tok = tokens[...].astype(F32)
    inverse = lax.rsqrt(jnp.mean(tok * tok, axis=-1, keepdims=True) + eps)
    normed_f = tok * inverse * mix_gain[...]
    normed = normed_f.astype(BF16)
    both = jnp.concatenate([normed.astype(F32), tok], axis=0).astype(BF16)
    for e in range(ep):
        send_a[e] = both[:, e * col : (e + 1) * col]
    recv_a[me] = send_a[me]

    pl.semaphore_wait(barrier, ep * tp - 1)

    order = sorted(range(1, ep), key=lambda k: -min(k, ep - k))
    near = order[::-1]
    for k in order:
        copy = to_ep(0, k, send_a.at[lax.rem(me + k, ep)], recv_a.at[me])
        copy.start()
        sends.append(copy)

    last = (((1,), (1,)), ((), ()))
    gate_all = lax.dot_general(normed, w_in_t[...], last, preferred_element_type=F32)
    pre = lax.dot_general(normed, w_forget_t[...], last, preferred_element_type=F32)
    pre = pre + forget_bias[...]
    forget_all = jnp.minimum(pre, 0.0) - jnp.log1p(jnp.exp(-jnp.abs(pre)))
    lane = lax.broadcasted_iota(jnp.int32, gate_all.shape, 1)
    decays, inflows, new_ms = [], [], []
    for h in range(heads):
        here = lane == mt * heads + h
        in_gate = jnp.sum(jnp.where(here, gate_all, 0.0), axis=1, keepdims=True)
        forget = jnp.sum(jnp.where(here, forget_all, 0.0), axis=1, keepdims=True)
        kept = forget + state_m[:, h : h + 1]
        top = jnp.maximum(kept, in_gate)
        new_ms.append(top)
        decays.append(jnp.exp(kept - top))
        inflows.append(jnp.exp(in_gate - top))
    for h in range(heads):
        out_m[:, h : h + 1] = new_ms[h]

    def piece(total, e):
        return total[e * seqs : (e + 1) * seqs]

    for name in ("q", "k", "v"):
        copies[name].wait()
    for k in near:
        to_ep(0, k, send_a.at[0], recv_a.at[source(k)]).wait_recv()
    arrived = [recv_a[e].astype(F32) for e in range(ep)]
    rows = jnp.concatenate([a[:seqs] for a in arrived], axis=0).astype(BF16)
    own_cols = jnp.concatenate([a[seqs:] for a in arrived], axis=0)
    part = jnp.dot(rows, v_qkv[...], preferred_element_type=F32)
    for e in range(ep):
        send_b[e] = piece(part, e).astype(BF16)
    recv_b[me] = send_b[me]
    for k in order:
        copy = to_ep(1, k, send_b.at[lax.rem(me + k, ep)], recv_b.at[me])
        copy.start()
        sends.append(copy)

    copies["c"].wait()
    for k in near:
        to_ep(1, k, send_b.at[0], recv_b.at[source(k)]).wait_recv()
    summed = recv_b[0].astype(F32)
    for e in range(1, ep):
        summed = summed + recv_b[e].astype(F32)
    summed = summed.astype(BF16).astype(F32)
    q_rows, k_rows, v_rows = [], [], []
    for s in range(seqs):
        for h in range(heads):
            row = summed[s : s + 1]
            q_rows.append(row[:, h * dqk : (h + 1) * dqk])
            k_rows.append(
                row[:, qk + h * dqk : qk + (h + 1) * dqk]
                * (dqk ** (-0.5) * inflows[h][s : s + 1])
            )
            v_rows.append(row[:, 2 * qk + h * dv : 2 * qk + (h + 1) * dv])
    upright = jnp.concatenate(q_rows + k_rows, axis=0).T
    count = seqs * heads
    head_rows = []
    for s in range(seqs):
        parts = []
        for h in range(heads):
            at = s * heads + h
            decay = decays[h][s : s + 1]
            q_col = upright[:, at : at + 1]
            k_col = upright[:, count + at : count + at + 1]
            fresh = decay * v_c[s, h] + k_col * v_rows[at]
            out_c[s, h] = fresh
            numer = jnp.sum(q_col * fresh, axis=0, keepdims=True)
            fresh_n = decay * state_n[s, h : h + 1] + k_rows[at]
            out_n[s, h : h + 1] = fresh_n
            denom = jnp.sum(q_rows[at] * fresh_n, axis=1, keepdims=True)
            parts.append(numer / jnp.maximum(jnp.abs(denom), 1.0))
        head_rows.append(jnp.concatenate(parts, axis=1))
    head_out = jnp.concatenate(head_rows, axis=0).astype(BF16)
    send_c[...] = head_out
    recv_c[me] = head_out
    for k in order:
        copy = to_ep(2, k, send_c, recv_c.at[me])
        copy.start()
        sends.append(copy)

    gate_rows = w_dense_gate[...].astype(F32)
    gate_row = jnp.concatenate(
        [gate_rows[i : i + 1] for i in range(width // 128)], axis=1
    )
    small = jnp.concatenate(
        [
            w_group_t[...].astype(F32),
            gate_row,
            jnp.zeros((8 - w_group_t.shape[0] - 1, width), F32),
        ],
        axis=0,
    ).astype(BF16)
    small_scr[...] = small

    copies["o"].wait()
    for k in near:
        to_ep(2, k, send_c, recv_c.at[source(k)]).wait_recv()
    all_heads = jnp.concatenate([recv_c[e].astype(F32) for e in range(ep)], axis=0).astype(BF16)
    out_part = jnp.dot(all_heads, v_out[...], preferred_element_type=F32).astype(BF16)
    send_d[...] = out_part
    recv_d[mt] = out_part

    def to_tp(j, dst):
        return pltpu.make_async_remote_copy(
            src_ref=send_d,
            dst_ref=dst,
            send_sem=tp_send.at[j],
            recv_sem=tp_recv.at[j],
            device_id={"ep": me, "tp": lax.rem(mt + j, tp)},
            device_id_type=MESH,
        )

    for j in range(1, tp):
        copy = to_tp(j, recv_d.at[mt])
        copy.start()
        sends.append(copy)
    for j in range(1, tp):
        to_tp(j, recv_d.at[lax.rem(mt + (tp - j), tp)]).wait_recv()
    mixer = recv_d[0].astype(F32)
    for j in range(1, tp):
        mixer = mixer + recv_d[j].astype(F32)
    residual = (own_cols + mixer).astype(BF16)
    blocks[me] = residual
    for k in order:
        copy = to_ep(3, k, blocks.at[me], blocks.at[me])
        copy.start()
        sends.append(copy)

    def gain_of(e):
        return moe_gain[:, pl.ds(pl.multiple_of(e * col, 128), col)]

    copies["d"].wait()
    scaled = (residual.astype(F32) * gain_of(me)).astype(BF16)
    dense_part = jnp.dot(scaled, v_dense[...], preferred_element_type=F32)
    for e in range(ep):
        send_g[e] = piece(dense_part, e).astype(BF16)
    recv_g[me] = send_g[me]
    for k in order:
        copy = to_ep(4, k, send_g.at[lax.rem(me + k, ep)], recv_g.at[me])
        copy.start()
        sends.append(copy)

    for name in ("g", "u", "w"):
        copies[name].wait()

    def block_terms(e, block):
        wide = block.astype(F32)
        squares = jnp.sum(wide * wide, axis=1, keepdims=True)
        scaled = (wide * gain_of(e)).astype(BF16)
        first = pl.multiple_of(e * col, 128)
        act = jnp.dot(scaled, v_gu[pl.ds(first, col), :], preferred_element_type=F32)
        logit = lax.dot_general(
            scaled, small_scr[:, pl.ds(first, col)], last, preferred_element_type=F32
        )
        return squares, act, logit

    squares, act, logit = block_terms(me, residual)
    for k in near:
        e = source(k)
        to_ep(3, k, blocks.at[me], blocks.at[e]).wait_recv()
        more = block_terms(e, blocks[e])
        squares, act, logit = squares + more[0], act + more[1], logit + more[2]
    factor = lax.rsqrt(squares * (1.0 / width) + eps)
    act = act * factor
    gate = act[:, :ff]
    hidden = (gate * jax.nn.sigmoid(gate) * act[:, ff:]).astype(BF16)
    down = jnp.dot(hidden, v_down[...], preferred_element_type=F32)
    for e in range(ep):
        for j in range(tp):
            send_f[e, j] = piece(down, e)[:, j * share : (j + 1) * share].astype(BF16)

    def final(k, j, dst):
        return pltpu.make_async_remote_copy(
            src_ref=send_f.at[lax.rem(me + k, ep), lax.rem(mt + j, tp)],
            dst_ref=dst,
            send_sem=f_send.at[k, j],
            recv_sem=f_recv.at[k, j],
            device_id={"ep": lax.rem(me + k, ep), "tp": lax.rem(mt + j, tp)},
            device_id_type=MESH,
        )

    for k in order + [0]:
        for j in range(tp):
            if k or j:
                copy = final(k, j, recv_f.at[me, mt])
                copy.start()
                sends.append(copy)
    recv_f[me, mt] = send_f[me, mt]

    groups = w_group_t.shape[0]
    spread = jnp.concatenate(
        [logit * factor, factor, jnp.zeros((every, 128 - 9), F32)]
        + [blocks[mt * (share // col) + i].astype(F32) for i in range(share // col)],
        axis=1,
    )
    for e in range(ep):
        rows_scr[e] = piece(spread, e)
    own = rows_scr[me]
    group_logit = own[:, :groups]
    dense_gate = jax.nn.sigmoid(own[:, groups : groups + 1]) * own[:, 8:9]
    shifted = jnp.exp(group_logit - jnp.max(group_logit, axis=1, keepdims=True))
    prob = shifted / jnp.sum(shifted, axis=1, keepdims=True)
    group_lane = lax.broadcasted_iota(jnp.int32, prob.shape, 1)
    per_group = ep // groups
    top_count = ids.shape[1]
    weights = weight[...]
    total_weight = jnp.sum(weights, axis=1, keepdims=True)
    lane_e = lax.broadcasted_iota(jnp.int32, (seqs, ep), 1)
    factor_e = jnp.zeros((seqs, ep), F32)
    for j in range(top_count):
        ident = ids[:, j : j + 1]
        picked = jnp.zeros((seqs, 1), F32)
        for g in range(groups):
            inside = (ident >= g * per_group) & (ident < (g + 1) * per_group)
            picked = picked + jnp.where(inside, prob[:, g : g + 1], 0.0)
        route = picked * weights[:, j : j + 1] / total_weight
        factor_e = factor_e + jnp.where(lane_e == ident, route, 0.0)

    for k in near:
        to_ep(4, k, send_g.at[0], recv_g.at[source(k)]).wait_recv()
    dense = recv_g[0].astype(F32)
    for e in range(1, ep):
        dense = dense + recv_g[e].astype(F32)
    result = own[:, 128:] + dense_gate * dense

    for k in [0] + near:
        for j in range(tp):
            if k or j:
                final(k, j, recv_f.at[source(k), lax.rem(mt + (tp - j), tp)]).wait_recv()
    for e in range(ep):
        expert = recv_f[e, 0].astype(F32)
        for j in range(1, tp):
            expert = expert + recv_f[e, j].astype(F32)
        result = result + factor_e[:, e : e + 1] * expert.astype(BF16).astype(F32)
    mixed[...] = result.astype(BF16)

    for copy in sends:
        copy.wait_send()


def fused(ep, tp, *args):
    (tokens, state_c, state_n, state_m, mix_gain, w_query, w_key, w_value) = args[:8]
    (w_in, w_forget, forget_bias, w_output, moe_gain, w_group, ids, weight) = args[8:16]
    (w_gate, w_up, w_down, w_dense, w_dense_gate) = args[16:]
    seqs, width = tokens.shape
    qk, vals = w_query.shape[1], w_value.shape[1]
    col, share, ff = width // ep, width // tp, w_gate.shape[2]
    every = seqs * ep
    wide = 2 * qk + vals
    vmem = pl.BlockSpec(memory_space=pltpu.VMEM)
    hbm = pl.BlockSpec(memory_space=pltpu.HBM)
    operands = [
        (tokens, vmem),
        (state_c, hbm),
        (state_n, vmem),
        (state_m, vmem),
        (mix_gain.reshape(1, width), vmem),
        (w_query, hbm),
        (w_key, hbm),
        (w_value, hbm),
        (w_in.T, vmem),
        (w_forget.T, vmem),
        (forget_bias.reshape(1, -1), vmem),
        (w_output, hbm),
        (moe_gain.reshape(1, width), vmem),
        (w_group.T, vmem),
        (ids, vmem),
        (weight, vmem),
        (w_gate, hbm),
        (w_up, hbm),
        (w_down, hbm),
        (w_dense, hbm),
        (w_dense_gate.reshape(-1, 128), vmem),
    ]
    scratch = [
        pltpu.VMEM(state_c.shape, F32),
        pltpu.VMEM((col, wide), BF16),
        pltpu.VMEM(w_output.shape, BF16),
        pltpu.VMEM((width, 2 * ff), BF16),
        pltpu.VMEM((ff, width), BF16),
        pltpu.VMEM(w_dense.shape, BF16),
        pltpu.VMEM((ep, 2 * seqs, col), BF16),
        pltpu.VMEM((ep, 2 * seqs, col), BF16),
        pltpu.VMEM((ep, seqs, wide), BF16),
        pltpu.VMEM((ep, seqs, wide), BF16),
        pltpu.VMEM((seqs, vals), BF16),
        pltpu.VMEM((ep, seqs, vals), BF16),
        pltpu.VMEM((every, col), BF16),
        pltpu.VMEM((tp, every, col), BF16),
        pltpu.VMEM((ep, every, col), BF16),
        pltpu.VMEM((ep, seqs, share), BF16),
        pltpu.VMEM((ep, seqs, share), BF16),
        pltpu.VMEM((ep, tp, seqs, share), BF16),
        pltpu.VMEM((ep, tp, seqs, share), BF16),
        pltpu.VMEM((ep, seqs, 128 + share), F32),
        pltpu.VMEM((8, width), BF16),
        pltpu.SemaphoreType.DMA((10,)),
        pltpu.SemaphoreType.DMA((5, ep)),
        pltpu.SemaphoreType.DMA((5, ep)),
        pltpu.SemaphoreType.DMA((tp,)),
        pltpu.SemaphoreType.DMA((tp,)),
        pltpu.SemaphoreType.DMA((ep, tp)),
        pltpu.SemaphoreType.DMA((ep, tp)),
    ]
    outs = (
        jax.ShapeDtypeStruct((seqs, share), BF16),
        jax.ShapeDtypeStruct(state_c.shape, F32),
        jax.ShapeDtypeStruct(state_n.shape, F32),
        jax.ShapeDtypeStruct(state_m.shape, F32),
    )
    spare = 4 * state_c.size + (20 << 10)
    kept = pl.pallas_call(
        functools.partial(step_kernel, ep, tp),
        out_shape=tuple(pltpu.VMEM(out.shape, out.dtype) for out in outs),
        in_specs=[spec for _, spec in operands],
        out_specs=(vmem,) * 4,
        scratch_shapes=scratch,
        compiler_params=pltpu.CompilerParams(
            collective_id=0, has_side_effects=True, vmem_limit_bytes=67043328 - spare
        ),
    )(*[value for value, _ in operands])
    return pl.pallas_call(
        write_out,
        out_shape=outs,
        in_specs=[vmem] * 4,
        out_specs=(pl.BlockSpec(memory_space=pltpu.HBM),) * 4,
        scratch_shapes=[pltpu.SemaphoreType.DMA((4,))],
        compiler_params=pltpu.CompilerParams(vmem_limit_bytes=4 << 20),
    )(*kept)


def write_out(*refs):
    sems = refs[-1]
    copies = [pltpu.make_async_copy(refs[i], refs[4 + i], sems.at[i]) for i in range(4)]
    for copy in copies:
        copy.start()
    for copy in copies:
        copy.wait()


def solution(mesh):
    ep, tp = mesh.shape["ep"], mesh.shape["tp"]

    def body(*args):
        return fused(ep, tp, *args) if fits(ep, tp, args) else per_device(*args)

    placed = (
        P("ep", None),
        P("ep", "tp", None, None),
        P("ep", "tp", None),
        P("ep", "tp"),
        P(),
        P("ep", "tp"),
        P("ep", "tp"),
        P("ep", "tp"),
        P(),
        P(),
        P(),
        P("tp", "ep"),
        P(),
        P(),
        P("ep", None),
        P("ep", None),
        P("ep", None, "tp"),
        P("ep", None, "tp"),
        P("ep", "tp", None),
        P("ep", "tp"),
        P(),
    )
    return jax.shard_map(
        body,
        mesh=mesh,
        in_specs=placed,
        out_specs=(P("ep", "tp"), P("ep", "tp", None, None), P("ep", "tp", None), P("ep", "tp")),
        check_vma=False,
    )
```

```python
import functools

import jax
import jax.numpy as jnp
from jax import lax
from jax.experimental import pallas as pl
from jax.experimental.pallas import tpu as pltpu
from jax.sharding import PartitionSpec as P

CAP = 1


eps = 1e-06


def rms_norm(values, gain):
    widened = values.astype(jnp.float32)
    inverse = lax.rsqrt(jnp.mean(widened * widened, axis=-1, keepdims=True) + eps)
    return (widened * inverse * gain).astype(jnp.bfloat16)


def rounded(values):
    return lax.optimization_barrier(values.astype(jnp.bfloat16)).astype(jnp.float32)


def memory_step(query_rows, key_rows, value_rows, in_gate, forget, state_c, state_n, state_m):
    seq_count, head_count = state_m.shape
    q_heads = query_rows.reshape(seq_count, head_count, -1)
    k_heads = key_rows.reshape(seq_count, head_count, -1) * q_heads.shape[-1] ** (-0.5)
    v_heads = value_rows.reshape(seq_count, head_count, -1)
    new_m = jnp.maximum(forget + state_m, in_gate)
    decay = jnp.exp(forget + state_m - new_m)
    inflow = jnp.exp(in_gate - new_m)
    new_c = (
        decay[..., None, None] * state_c
        + (inflow[..., None] * k_heads)[..., :, None] * v_heads[..., None, :]
    )
    new_n = decay[..., None] * state_n + inflow[..., None] * k_heads
    numer = jnp.einsum("shd,shde->she", q_heads, new_c, precision=lax.Precision.HIGHEST)
    denom = jnp.maximum(jnp.abs(jnp.sum(q_heads * new_n, axis=-1)), 1.0)
    heads = (numer / denom[..., None]).astype(jnp.bfloat16).reshape(seq_count, -1)
    return (heads, new_c, new_n, new_m)


def per_device(
    tokens,
    state_c,
    state_n,
    state_m,
    mix_gain,
    w_query,
    w_key,
    w_value,
    w_input_gate,
    w_forget_gate,
    forget_bias,
    w_output,
    moe_gain,
    w_group,
    expert_ids,
    expert_weight,
    w_exp_gate,
    w_exp_up,
    w_exp_down,
    w_dense,
    w_dense_gate,
):
    seq_count = tokens.shape[0]
    width = tokens.shape[1]
    tp_count = lax.axis_size("tp")
    ep_count = lax.axis_size("ep")
    tp_rank = lax.axis_index("tp")
    head_count = state_m.shape[1]
    qk_cols = w_query.shape[1]
    share = width // tp_count
    normed = rms_norm(tokens, mix_gain)
    spread_cols = lax.all_to_all(normed, "ep", split_axis=1, concat_axis=0, tiled=True)
    joined = jnp.concatenate([w_query, w_key, w_value], axis=1)
    token_rows = spread_cols
    summed = lax.psum_scatter(
        jnp.dot(token_rows, joined, preferred_element_type=jnp.float32),
        "ep",
        scatter_dimension=0,
        tiled=True,
    )
    query_sum = summed[:, :qk_cols]
    key_sum = summed[:, qk_cols : 2 * qk_cols]
    value_sum = summed[:, 2 * qk_cols :]
    query_rows = rounded(query_sum)
    key_rows = rounded(key_sum)
    value_rows = rounded(value_sum)
    gate_all = jnp.dot(normed, w_input_gate, preferred_element_type=jnp.float32)
    forget_all = jax.nn.log_sigmoid(
        jnp.dot(normed, w_forget_gate, preferred_element_type=jnp.float32) + forget_bias
    )
    in_gate = lax.dynamic_slice_in_dim(gate_all, tp_rank * head_count, head_count, 1)
    forget = lax.dynamic_slice_in_dim(forget_all, tp_rank * head_count, head_count, 1)
    heads, new_c, new_n, new_m = memory_step(
        query_rows, key_rows, value_rows, in_gate, forget, state_c, state_n, state_m
    )
    row_parts = jnp.dot(
        lax.all_gather(heads, "ep", axis=0, tiled=True),
        w_output,
        preferred_element_type=jnp.float32,
    ).astype(jnp.bfloat16)
    partial_value = lax.all_to_all(row_parts, "ep", split_axis=0, concat_axis=1, tiled=True).astype(
        jnp.float32
    )
    mixer_sum = lax.psum(partial_value.astype(jnp.bfloat16), "tp").astype(jnp.float32)
    residual = (tokens.astype(jnp.float32) + mixer_sum).astype(jnp.bfloat16)
    normed2 = rms_norm(residual, moe_gain)
    group_count = w_group.shape[1]
    group_prob = jax.nn.softmax(
        jnp.dot(normed2, w_group, preferred_element_type=jnp.float32), axis=-1
    )
    experts_here = w_exp_gate.shape[0]
    expert_count = experts_here * ep_count
    per_group = expert_count // group_count
    top_count = expert_ids.shape[1]
    member = (expert_ids // per_group)[..., None] == jnp.arange(group_count, dtype=jnp.int32)[
        None, None, :
    ]
    picked = jnp.sum(jnp.where(member, group_prob[:, None, :], 0.0), axis=-1)
    route = picked * expert_weight / jnp.sum(expert_weight, axis=1, keepdims=True)
    flat_ids = expert_ids.reshape(-1)
    assigned = flat_ids[:, None] == jnp.arange(expert_count, dtype=jnp.int32)[None, :]
    ranks = jnp.cumsum(assigned.astype(jnp.int32), axis=0) - 1
    own_rank = jnp.sum(jnp.where(assigned, ranks, 0), axis=1)
    slot_index = flat_ids * CAP + own_rank
    placing = (
        jnp.arange(expert_count * CAP, dtype=jnp.int32)[:, None] == slot_index[None, :]
    ).astype(jnp.bfloat16)
    repeated = jnp.repeat(normed2, top_count, axis=0)
    outgoing = jnp.dot(placing, repeated, preferred_element_type=jnp.float32).astype(jnp.bfloat16)
    outgoing = outgoing.reshape(expert_count, CAP, width)
    arrived = lax.all_to_all(outgoing, "ep", split_axis=0, concat_axis=0, tiled=True)
    slots = arrived.shape[1]
    grid_rows = arrived.reshape(ep_count, experts_here, slots, width)
    gate_act = jnp.einsum(
        "sxnd,xdf->sxnf", grid_rows, w_exp_gate, preferred_element_type=jnp.float32
    )
    up_act = jnp.einsum("sxnd,xdf->sxnf", grid_rows, w_exp_up, preferred_element_type=jnp.float32)
    hidden = (jax.nn.silu(gate_act) * up_act).astype(jnp.bfloat16)
    down_part = jnp.einsum("sxnf,xfd->sxnd", hidden, w_exp_down, preferred_element_type=jnp.float32)
    reduced = lax.psum_scatter(
        down_part.astype(jnp.bfloat16), "tp", scatter_dimension=3, tiled=True
    )
    returned = lax.all_to_all(
        reduced.reshape(expert_count, slots, share), "ep", split_axis=0, concat_axis=0, tiled=True
    )
    picked_rows = jnp.einsum(
        "ca,cd->ad",
        placing,
        returned.reshape(expert_count * CAP, share),
        preferred_element_type=jnp.float32,
    )
    moe = jnp.sum(route[..., None] * picked_rows.reshape(seq_count, top_count, share), axis=1)
    dense_cols = lax.all_to_all(normed2, "ep", split_axis=1, concat_axis=0, tiled=True)
    token_rows = dense_cols
    dense_raw = lax.psum_scatter(
        jnp.dot(token_rows, w_dense, preferred_element_type=jnp.float32),
        "ep",
        scatter_dimension=0,
        tiled=True,
    )
    dense_gate = jax.nn.sigmoid(jnp.dot(normed2, w_dense_gate, preferred_element_type=jnp.float32))
    own_cols = lax.dynamic_slice_in_dim(residual, tp_rank * share, share, 1).astype(jnp.float32)
    mixed = (own_cols + moe + dense_gate[:, None] * dense_raw).astype(jnp.bfloat16)
    return (mixed, new_c, new_n, new_m)


SMALL = (0, 2, 3, 4, 8, 9, 10, 12, 13, 14, 15, 20)
F32 = jnp.float32
BF16 = jnp.bfloat16
MESH = pl.DeviceIdType.MESH


def fits(ep, tp, args):
    tokens, state_c, w_query, w_exp_gate = args[0], args[1], args[5], args[16]
    seqs, width = tokens.shape
    dqk, dv = state_c.shape[2:]
    return (
        width % (ep * 128) == 0
        and ep % tp == 0
        and w_query.shape[1] % 128 == 0
        and dqk % 128 == 0
        and dv % 128 == 0
        and (width // tp) % 128 == 0
        and w_exp_gate.shape[0] == 1
        and w_exp_gate.shape[2] % 128 == 0
        and seqs == 2
    )


def step_kernel(
    ep,
    tp,
    h_tokens,
    state_c,
    h_state_n,
    h_state_m,
    h_mix_gain,
    w_query,
    w_key,
    w_value,
    h_w_in_t,
    h_w_forget_t,
    h_forget_bias,
    w_output,
    h_moe_gain,
    h_w_group_t,
    h_ids,
    h_weight,
    w_gate,
    w_up,
    w_down,
    w_dense,
    h_w_dense_gate,
    mixed,
    out_c,
    out_n,
    out_m,
    tokens,
    state_n,
    state_m,
    mix_gain,
    w_in_t,
    w_forget_t,
    forget_bias,
    moe_gain,
    w_group_t,
    ids,
    weight,
    w_dense_gate,
    v_c,
    v_qkv,
    v_out,
    v_gu,
    v_down,
    v_dense,
    send_a,
    recv_a,
    send_b,
    recv_b,
    send_c,
    recv_c,
    send_d,
    recv_d,
    blocks,
    send_g,
    recv_g,
    send_f,
    recv_f,
    rows_scr,
    small_scr,
    local_sem,
    ep_send,
    ep_recv,
    tp_send,
    tp_recv,
    f_send,
    f_recv,
):
    me = lax.axis_index("ep")
    mt = lax.axis_index("tp")
    seqs, width = tokens.shape
    heads = state_c.shape[1]
    dqk, dv = state_c.shape[2:]
    qk = heads * dqk
    col = width // ep
    share = width // tp
    ff = w_gate.shape[2]
    every = ep * seqs

    barrier = pltpu.get_barrier_semaphore()
    for k in range(ep):
        for j in range(tp):
            if (k == 0) != (j == 0):
                pl.semaphore_signal(
                    barrier,
                    inc=1,
                    device_id={"ep": lax.rem(me + k, ep), "tp": lax.rem(mt + j, tp)},
                    device_id_type=MESH,
                )

    copies = {}
    plan = [
        ("tokens", h_tokens, tokens),
        ("mix_gain", h_mix_gain, mix_gain),
        ("q", w_query, v_qkv.at[:, 0:qk]),
        ("k", w_key, v_qkv.at[:, qk : 2 * qk]),
        ("v", w_value, v_qkv.at[:, 2 * qk :]),
        ("w_in_t", h_w_in_t, w_in_t),
        ("w_forget_t", h_w_forget_t, w_forget_t),
        ("forget_bias", h_forget_bias, forget_bias),
        ("state_m", h_state_m, state_m),
        ("c", state_c, v_c),
        ("state_n", h_state_n, state_n),
        ("o", w_output, v_out),
        ("d", w_dense, v_dense),
        ("g", w_gate.at[0], v_gu.at[:, 0:ff]),
        ("u", w_up.at[0], v_gu.at[:, ff:]),
        ("w", w_down.at[0], v_down),
        ("moe_gain", h_moe_gain, moe_gain),
        ("w_group_t", h_w_group_t, w_group_t),
        ("w_dense_gate", h_w_dense_gate, w_dense_gate),
        ("ids", h_ids, ids),
        ("weight", h_weight, weight),
    ]
    for number, (name, src, dst) in enumerate(plan):
        copies[name] = pltpu.make_async_copy(src, dst, local_sem.at[number])
        copies[name].start()

    def to_ep(phase, k, src, dst):
        return pltpu.make_async_remote_copy(
            src_ref=src,
            dst_ref=dst,
            send_sem=ep_send.at[phase, k],
            recv_sem=ep_recv.at[phase, k],
            device_id={"ep": lax.rem(me + k, ep), "tp": mt},
            device_id_type=MESH,
        )

    def source(k):
        return lax.rem(me + (ep - k), ep)

    sends = []
    copies["tokens"].wait()
    copies["mix_gain"].wait()
    tok = tokens[...].astype(F32)
    inverse = lax.rsqrt(jnp.mean(tok * tok, axis=-1, keepdims=True) + eps)
    normed_f = tok * inverse * mix_gain[...]
    normed = normed_f.astype(BF16)
    both = jnp.concatenate([normed.astype(F32), tok], axis=0).astype(BF16)
    for e in range(ep):
        send_a[e] = both[:, e * col : (e + 1) * col]
    recv_a[me] = send_a[me]

    pl.semaphore_wait(barrier, ep + tp - 2)

    order = sorted(range(1, ep), key=lambda k: -min(k, ep - k))
    near = order[::-1]
    for k in order:
        copy = to_ep(0, k, send_a.at[lax.rem(me + k, ep)], recv_a.at[me])
        copy.start()
        sends.append(copy)

    for name in ("w_in_t", "w_forget_t", "forget_bias", "state_m"):
        copies[name].wait()
    last = (((1,), (1,)), ((), ()))
    gate_all = lax.dot_general(normed, w_in_t[...], last, preferred_element_type=F32)
    pre = lax.dot_general(normed, w_forget_t[...], last, preferred_element_type=F32)
    pre = pre + forget_bias[...]
    forget_all = jnp.minimum(pre, 0.0) - jnp.log1p(jnp.exp(-jnp.abs(pre)))
    lane = lax.broadcasted_iota(jnp.int32, gate_all.shape, 1)
    decays, inflows, new_ms = [], [], []
    for h in range(heads):
        here = lane == mt * heads + h
        in_gate = jnp.sum(jnp.where(here, gate_all, 0.0), axis=1, keepdims=True)
        forget = jnp.sum(jnp.where(here, forget_all, 0.0), axis=1, keepdims=True)
        kept = forget + state_m[:, h : h + 1]
        top = jnp.maximum(kept, in_gate)
        new_ms.append(top)
        decays.append(jnp.exp(kept - top))
        inflows.append(jnp.exp(in_gate - top))
    for h in range(heads):
        out_m[:, h : h + 1] = new_ms[h]

    def piece(total, e):
        return total[e * seqs : (e + 1) * seqs]

    for name in ("q", "k", "v"):
        copies[name].wait()
    for k in near:
        to_ep(0, k, send_a.at[0], recv_a.at[source(k)]).wait_recv()
    arrived = [recv_a[e].astype(F32) for e in range(ep)]
    rows = jnp.concatenate([a[:seqs] for a in arrived], axis=0).astype(BF16)
    own_cols = jnp.concatenate([a[seqs:] for a in arrived], axis=0)
    part = jnp.dot(rows, v_qkv[...], preferred_element_type=F32)
    for e in range(ep):
        send_b[e] = piece(part, e).astype(BF16)
    recv_b[me] = send_b[me]
    for k in order:
        copy = to_ep(1, k, send_b.at[lax.rem(me + k, ep)], recv_b.at[me])
        copy.start()
        sends.append(copy)

    copies["c"].wait()
    copies["state_n"].wait()
    for k in near:
        to_ep(1, k, send_b.at[0], recv_b.at[source(k)]).wait_recv()
    summed = recv_b[0].astype(F32)
    for e in range(1, ep):
        summed = summed + recv_b[e].astype(F32)
    summed = summed.astype(BF16).astype(F32)
    q_rows, k_rows, v_rows = [], [], []
    for s in range(seqs):
        for h in range(heads):
            row = summed[s : s + 1]
            q_rows.append(row[:, h * dqk : (h + 1) * dqk])
            k_rows.append(
                row[:, qk + h * dqk : qk + (h + 1) * dqk]
                * (dqk ** (-0.5) * inflows[h][s : s + 1])
            )
            v_rows.append(row[:, 2 * qk + h * dv : 2 * qk + (h + 1) * dv])
    upright = jnp.concatenate(q_rows + k_rows, axis=0).T
    count = seqs * heads
    head_rows = []
    for s in range(seqs):
        parts = []
        for h in range(heads):
            at = s * heads + h
            decay = decays[h][s : s + 1]
            q_col = upright[:, at : at + 1]
            k_col = upright[:, count + at : count + at + 1]
            fresh = decay * v_c[s, h] + k_col * v_rows[at]
            out_c[s, h] = fresh
            numer = jnp.sum(q_col * fresh, axis=0, keepdims=True)
            fresh_n = decay * state_n[s, h : h + 1] + k_rows[at]
            out_n[s, h : h + 1] = fresh_n
            denom = jnp.sum(q_rows[at] * fresh_n, axis=1, keepdims=True)
            parts.append(numer / jnp.maximum(jnp.abs(denom), 1.0))
        head_rows.append(jnp.concatenate(parts, axis=1))
    head_out = jnp.concatenate(head_rows, axis=0).astype(BF16)
    send_c[...] = head_out
    recv_c[me] = head_out
    for k in order:
        copy = to_ep(2, k, send_c, recv_c.at[me])
        copy.start()
        sends.append(copy)

    for name in ("moe_gain", "w_group_t", "w_dense_gate", "ids", "weight"):
        copies[name].wait()
    gate_rows = w_dense_gate[...].astype(F32)
    gate_row = jnp.concatenate(
        [gate_rows[i : i + 1] for i in range(width // 128)], axis=1
    )
    small = jnp.concatenate(
        [
            w_group_t[...].astype(F32),
            gate_row,
            jnp.zeros((8 - w_group_t.shape[0] - 1, width), F32),
        ],
        axis=0,
    ).astype(BF16)
    small_scr[...] = small

    copies["o"].wait()
    for k in near:
        to_ep(2, k, send_c, recv_c.at[source(k)]).wait_recv()
    all_heads = jnp.concatenate([recv_c[e].astype(F32) for e in range(ep)], axis=0).astype(BF16)
    out_part = jnp.dot(all_heads, v_out[...], preferred_element_type=F32).astype(BF16)
    send_d[...] = out_part
    recv_d[mt] = out_part

    def to_tp(j, dst):
        return pltpu.make_async_remote_copy(
            src_ref=send_d,
            dst_ref=dst,
            send_sem=tp_send.at[j],
            recv_sem=tp_recv.at[j],
            device_id={"ep": me, "tp": lax.rem(mt + j, tp)},
            device_id_type=MESH,
        )

    for j in range(1, tp):
        copy = to_tp(j, recv_d.at[mt])
        copy.start()
        sends.append(copy)
    for j in range(1, tp):
        to_tp(j, recv_d.at[lax.rem(mt + (tp - j), tp)]).wait_recv()
    mixer = recv_d[0].astype(F32)
    for j in range(1, tp):
        mixer = mixer + recv_d[j].astype(F32)
    residual = (own_cols + mixer).astype(BF16)
    blocks[me] = residual
    for k in order:
        copy = to_ep(3, k, blocks.at[me], blocks.at[me])
        copy.start()
        sends.append(copy)

    def gain_of(e):
        return moe_gain[:, pl.ds(pl.multiple_of(e * col, 128), col)]

    copies["d"].wait()
    scaled = (residual.astype(F32) * gain_of(me)).astype(BF16)
    dense_part = jnp.dot(scaled, v_dense[...], preferred_element_type=F32)
    for e in range(ep):
        send_g[e] = piece(dense_part, e).astype(BF16)
    recv_g[me] = send_g[me]
    for k in order:
        copy = to_ep(4, k, send_g.at[lax.rem(me + k, ep)], recv_g.at[me])
        copy.start()
        sends.append(copy)

    for name in ("g", "u", "w"):
        copies[name].wait()

    def block_terms(e, block):
        wide = block.astype(F32)
        squares = jnp.sum(wide * wide, axis=1, keepdims=True)
        scaled = (wide * gain_of(e)).astype(BF16)
        first = pl.multiple_of(e * col, 128)
        act = jnp.dot(scaled, v_gu[pl.ds(first, col), :], preferred_element_type=F32)
        logit = lax.dot_general(
            scaled, small_scr[:, pl.ds(first, col)], last, preferred_element_type=F32
        )
        return squares, act, logit

    squares, act, logit = block_terms(me, residual)
    for k in near:
        e = source(k)
        to_ep(3, k, blocks.at[me], blocks.at[e]).wait_recv()
        more = block_terms(e, blocks[e])
        squares, act, logit = squares + more[0], act + more[1], logit + more[2]
    factor = lax.rsqrt(squares * (1.0 / width) + eps)
    act = act * factor
    gate = act[:, :ff]
    hidden = (gate * jax.nn.sigmoid(gate) * act[:, ff:]).astype(BF16)
    down = jnp.dot(hidden, v_down[...], preferred_element_type=F32)
    for e in range(ep):
        for j in range(tp):
            send_f[e, j] = piece(down, e)[:, j * share : (j + 1) * share].astype(BF16)

    def final(k, j, dst):
        return pltpu.make_async_remote_copy(
            src_ref=send_f.at[lax.rem(me + k, ep), lax.rem(mt + j, tp)],
            dst_ref=dst,
            send_sem=f_send.at[k, j],
            recv_sem=f_recv.at[k, j],
            device_id={"ep": lax.rem(me + k, ep), "tp": lax.rem(mt + j, tp)},
            device_id_type=MESH,
        )

    for k in order + [0]:
        for j in range(tp):
            if k or j:
                copy = final(k, j, recv_f.at[me, mt])
                copy.start()
                sends.append(copy)
    recv_f[me, mt] = send_f[me, mt]

    groups = w_group_t.shape[0]
    spread = jnp.concatenate(
        [logit * factor, factor, jnp.zeros((every, 128 - 9), F32)]
        + [blocks[mt * (share // col) + i].astype(F32) for i in range(share // col)],
        axis=1,
    )
    for e in range(ep):
        rows_scr[e] = piece(spread, e)
    own = rows_scr[me]
    group_logit = own[:, :groups]
    dense_gate = jax.nn.sigmoid(own[:, groups : groups + 1]) * own[:, 8:9]
    shifted = jnp.exp(group_logit - jnp.max(group_logit, axis=1, keepdims=True))
    prob = shifted / jnp.sum(shifted, axis=1, keepdims=True)
    group_lane = lax.broadcasted_iota(jnp.int32, prob.shape, 1)
    per_group = ep // groups
    top_count = ids.shape[1]
    weights = weight[...]
    total_weight = jnp.sum(weights, axis=1, keepdims=True)
    lane_e = lax.broadcasted_iota(jnp.int32, (seqs, ep), 1)
    factor_e = jnp.zeros((seqs, ep), F32)
    for j in range(top_count):
        ident = ids[:, j : j + 1]
        picked = jnp.zeros((seqs, 1), F32)
        for g in range(groups):
            inside = (ident >= g * per_group) & (ident < (g + 1) * per_group)
            picked = picked + jnp.where(inside, prob[:, g : g + 1], 0.0)
        route = picked * weights[:, j : j + 1] / total_weight
        factor_e = factor_e + jnp.where(lane_e == ident, route, 0.0)

    for k in near:
        to_ep(4, k, send_g.at[0], recv_g.at[source(k)]).wait_recv()
    dense = recv_g[0].astype(F32)
    for e in range(1, ep):
        dense = dense + recv_g[e].astype(F32)
    result = own[:, 128:] + dense_gate * dense

    for k in [0] + near:
        for j in range(tp):
            if k or j:
                final(k, j, recv_f.at[source(k), lax.rem(mt + (tp - j), tp)]).wait_recv()
    for e in range(ep):
        expert = recv_f[e, 0].astype(F32)
        for j in range(1, tp):
            expert = expert + recv_f[e, j].astype(F32)
        result = result + factor_e[:, e : e + 1] * expert.astype(BF16).astype(F32)
    mixed[...] = result.astype(BF16)

    for copy in sends:
        copy.wait_send()


def fused(ep, tp, *args):
    (tokens, state_c, state_n, state_m, mix_gain, w_query, w_key, w_value) = args[:8]
    (w_in, w_forget, forget_bias, w_output, moe_gain, w_group, ids, weight) = args[8:16]
    (w_gate, w_up, w_down, w_dense, w_dense_gate) = args[16:]
    seqs, width = tokens.shape
    qk, vals = w_query.shape[1], w_value.shape[1]
    col, share, ff = width // ep, width // tp, w_gate.shape[2]
    every = seqs * ep
    wide = 2 * qk + vals
    vmem = pl.BlockSpec(memory_space=pltpu.VMEM)
    hbm = pl.BlockSpec(memory_space=pltpu.HBM)
    operands = [
        (tokens, hbm),
        (state_c, hbm),
        (state_n, hbm),
        (state_m, hbm),
        (mix_gain.reshape(1, width), hbm),
        (w_query, hbm),
        (w_key, hbm),
        (w_value, hbm),
        (w_in.T, hbm),
        (w_forget.T, hbm),
        (forget_bias.reshape(1, -1), hbm),
        (w_output, hbm),
        (moe_gain.reshape(1, width), hbm),
        (w_group.T, hbm),
        (ids, hbm),
        (weight, hbm),
        (w_gate, hbm),
        (w_up, hbm),
        (w_down, hbm),
        (w_dense, hbm),
        (w_dense_gate.reshape(-1, 128), hbm),
    ]
    scratch = [pltpu.VMEM(operands[i][0].shape, operands[i][0].dtype) for i in SMALL] + [
        pltpu.VMEM(state_c.shape, F32),
        pltpu.VMEM((col, wide), BF16),
        pltpu.VMEM(w_output.shape, BF16),
        pltpu.VMEM((width, 2 * ff), BF16),
        pltpu.VMEM((ff, width), BF16),
        pltpu.VMEM(w_dense.shape, BF16),
        pltpu.VMEM((ep, 2 * seqs, col), BF16),
        pltpu.VMEM((ep, 2 * seqs, col), BF16),
        pltpu.VMEM((ep, seqs, wide), BF16),
        pltpu.VMEM((ep, seqs, wide), BF16),
        pltpu.VMEM((seqs, vals), BF16),
        pltpu.VMEM((ep, seqs, vals), BF16),
        pltpu.VMEM((every, col), BF16),
        pltpu.VMEM((tp, every, col), BF16),
        pltpu.VMEM((ep, every, col), BF16),
        pltpu.VMEM((ep, seqs, share), BF16),
        pltpu.VMEM((ep, seqs, share), BF16),
        pltpu.VMEM((ep, tp, seqs, share), BF16),
        pltpu.VMEM((ep, tp, seqs, share), BF16),
        pltpu.VMEM((ep, seqs, 128 + share), F32),
        pltpu.VMEM((8, width), BF16),
        pltpu.SemaphoreType.DMA((len(operands),)),
        pltpu.SemaphoreType.DMA((5, ep)),
        pltpu.SemaphoreType.DMA((5, ep)),
        pltpu.SemaphoreType.DMA((tp,)),
        pltpu.SemaphoreType.DMA((tp,)),
        pltpu.SemaphoreType.DMA((ep, tp)),
        pltpu.SemaphoreType.DMA((ep, tp)),
    ]
    outs = (
        jax.ShapeDtypeStruct((seqs, share), BF16),
        jax.ShapeDtypeStruct(state_c.shape, F32),
        jax.ShapeDtypeStruct(state_n.shape, F32),
        jax.ShapeDtypeStruct(state_m.shape, F32),
    )
    spare = 4 * state_c.size + (20 << 10)
    kept = pl.pallas_call(
        functools.partial(step_kernel, ep, tp),
        out_shape=tuple(pltpu.VMEM(out.shape, out.dtype) for out in outs),
        in_specs=[spec for _, spec in operands],
        out_specs=(vmem,) * 4,
        scratch_shapes=scratch,
        compiler_params=pltpu.CompilerParams(
            collective_id=0, has_side_effects=True, vmem_limit_bytes=67043328 - spare
        ),
    )(*[value for value, _ in operands])
    return pl.pallas_call(
        write_out,
        out_shape=outs,
        in_specs=[vmem] * 4,
        out_specs=(pl.BlockSpec(memory_space=pltpu.HBM),) * 4,
        scratch_shapes=[pltpu.SemaphoreType.DMA((4,))],
        compiler_params=pltpu.CompilerParams(vmem_limit_bytes=4 << 20),
    )(*kept)


def write_out(*refs):
    sems = refs[-1]
    copies = [pltpu.make_async_copy(refs[i], refs[4 + i], sems.at[i]) for i in range(4)]
    for copy in copies:
        copy.start()
    for copy in copies:
        copy.wait()


def solution(mesh):
    ep, tp = mesh.shape["ep"], mesh.shape["tp"]

    def body(*args):
        return fused(ep, tp, *args) if fits(ep, tp, args) else per_device(*args)

    placed = (
        P("ep", None),
        P("ep", "tp", None, None),
        P("ep", "tp", None),
        P("ep", "tp"),
        P(),
        P("ep", "tp"),
        P("ep", "tp"),
        P("ep", "tp"),
        P(),
        P(),
        P(),
        P("tp", "ep"),
        P(),
        P(),
        P("ep", None),
        P("ep", None),
        P("ep", None, "tp"),
        P("ep", None, "tp"),
        P("ep", "tp", None),
        P("ep", "tp"),
        P(),
    )
    return jax.shard_map(
        body,
        mesh=mesh,
        in_specs=placed,
        out_specs=(P("ep", "tp"), P("ep", "tp", None, None), P("ep", "tp", None), P("ep", "tp")),
        check_vma=False,
    )
```
